32 devices in a mesh: sp: 8 (over z, x), tp: 4 (over y, core).
Axes of the slice: x: 2, y: 2, z: 4, core: 2. Of those that a mesh axis runs over, the one named last changes fastest.
Arguments:
- stream: bfloat16 [4096, 2048], P(('sp', 'tp')), may hold values from -6 to 6
- projected: bfloat16 [4096, 2048], P('sp', 'tp'), may hold values from -6 to 6
- segments: int32 [4096], P('sp'), may hold values from 0 to 3, never falling along the last dimension, each value on 1 to 1536 neighbouring positions
- group_weight: bfloat16 [4, 512, 512], replicated, may hold values from -0.25 to 0.25
- group_scale: float32 [2048], replicated, may hold values from 0.1 to 1.9
- out_weight: bfloat16 [2048, 2048], replicated, may hold values from -0.125 to 0.125
- ffn_gain: float32 [2048], replicated, may hold values from 0.1 to 1.9
- routes: int32 [4096, 4], P(('sp', 'tp')), may hold values from 0 to 31, all different within a row; in each aligned block of 128 rows (0 to 127, 128 to 255, ...) at most 24 rows name the same one
- route_weights: float32 [4096, 4], P(('sp', 'tp')), may hold values from 0.05 to 0.5
- expert_gate: bfloat16 [32, 2048, 1024], P(('sp', 'tp')), may hold values from -0.25 to 0.25
- expert_up: bfloat16 [32, 2048, 1024], P(('sp', 'tp')), may hold values from -0.25 to 0.25
- expert_down: bfloat16 [32, 1024, 2048], P(('sp', 'tp')), may hold values from -0.1875 to 0.1875
Outputs:
- combined: bfloat16 [4096, 2048], P(('sp', 'tp'))
The draws below stay inside these ranges and needn't reach their ends.
Inputs may be any that keep to these rules, and one draw needn't show every extreme that they name: `segments`: document numbers never fall along the positions; a document has 1 to 1536 positions, and one has exactly 1536. `routes`: each row names 4 different experts. Among the 128 rows of one device (aligned blocks), no expert is named more than 24 times, and in some blocks one is named exactly 24 times.
All inputs are finite; a program needn't handle non-finite values.
Results may differ from the reference program's by a relative error of at most 0.015.
Values may be sent and summed in bfloat16 or wider, within the bound.
A program may use at most 128 MiB of HBM per device.

```python
import math
import jax
import jax.numpy as jnp
import numpy as np
from jax import lax

D = 2048
GROUPS = 4
FF = 1024
TOP = 4
TOK_DEV = 128
TOKENS = 4096
GROUP_WIDTH = 512
EXPERTS = 32
CAP = 24
DOCS = 4
DOC_MOST = 1536


def levels(key, extent, shards, low, high):
    def one(dim, shards_of):
        heights = jax.random.uniform(jax.random.fold_in(jax.random.fold_in(key, 6), dim), (shards_of,), jnp.float32, low / len(shards), high / len(shards))
        return jnp.repeat(jnp.exp(heights), extent[dim] // shards_of).reshape((-1,) + (1,) * (len(extent) - dim - 1))

    loudness = one(*shards[0])
    for cut in shards[1:]:
        loudness = loudness * one(*cut)
    return loudness


def split_up(count, total, bound, skew):
    loads = [(1 << 20) // math.isqrt(standing ** skew) + 1 for standing in range(2, count + 1)]
    rest, given = total - bound - (count - 1), [1] * (count - 1)
    while rest > 0:
        candidates = [i for i in range(count - 1) if given[i] < bound]
        pool, remaining = sum([loads[i] for i in candidates]), rest
        for i in candidates:
            extra = min(bound - given[i], max(1, remaining * loads[i] // pool), rest)
            given[i] = given[i] + extra
            rest = rest - extra
    return np.array([bound] + given)


def ragged_sizes(own_key, number_of, total, most, skew):
    if number_of == 2:
        one = jax.random.randint(own_key, (), max(1, total - most), min(most, total - 1) + 1)
        return jnp.stack([one, total - one])
    lengths = jnp.asarray(split_up(number_of, total, most, skew), jnp.int32)
    couples = (number_of - 1) // 2
    source_of, taker = lengths[1:1 + 2 * couples:2], lengths[2:2 + 2 * couples:2]
    room = jnp.minimum(source_of - 1, most - taker)
    passed = jax.random.randint(jax.random.fold_in(own_key, 1), (couples,), 0, 1 << 20) % (room + 1)
    lengths = lengths.at[1:1 + 2 * couples:2].set(source_of - passed).at[2:2 + 2 * couples:2].set(taker + passed)
    return lengths[jax.random.permutation(jax.random.fold_in(own_key, 2), number_of)]


def deal_out(own_key, own, number, rows, number_of, top, most, lean):
    ranking = jax.random.permutation(own_key, number_of)
    crowded, usual = load_shares(number_of, rows * top, most, lean, True), load_shares(number_of, rows * top, most, lean, False)
    places = jnp.arange(number_of)

    def named(lengths, turn):
        used = int((lengths > 0).sum())
        fixed = max(1, used // 4)
        passed = fixed + (places - fixed + turn * (used - fixed)) % max(1, number_of - fixed)
        return jnp.zeros((number_of,), jnp.int32).at[ranking[jnp.where(places < fixed, places, passed)]].set(jnp.asarray(lengths, jnp.int32))

    lengths = jnp.where(number % 4 == 0, named(crowded, number // 4), named(usual, number - number // 4 - 1))
    mixed = jax.random.permutation(jax.random.fold_in(own, 3), number_of)
    giver, taker = mixed[0:number_of // 2 * 2:2], mixed[1:number_of // 2 * 2:2]
    margin = jnp.minimum(lengths[giver] - 1, most - lengths[taker]) // 2
    margin = jnp.where((giver == ranking[0]) | (taker == ranking[0]) | (lengths[taker] == 0), 0, jnp.maximum(margin, 0))
    passed = jax.random.randint(jax.random.fold_in(own, 4), (number_of // 2,), 0, 1 << 20) % (margin + 1)
    lengths = lengths.at[giver].add(-passed).at[taker].add(passed)
    labels = jnp.searchsorted(jnp.cumsum(lengths), jnp.arange(rows * top), side="right").astype(jnp.int32)
    table = labels.reshape(top, rows).T
    table = table[jax.random.permutation(jax.random.fold_in(own, 1), rows)]
    turn = jax.random.randint(jax.random.fold_in(own, 2), (rows, 1), 0, top)
    return jnp.take_along_axis(table, (jnp.arange(top)[None, :] + turn) % top, axis=1)


def load_shares(count, total, limit, skew, full):
    weights = [(1 << 20) // math.isqrt(rank ** skew) + 1 for rank in range(1, count + 1)]
    largest = limit if full else min(limit, max(-(-total // count), total * weights[0] // sum(weights)))
    least = 1 if total - largest >= count - 1 else 0
    holding, rest = [largest] + [least] * (count - 1), total - largest - least * (count - 1)
    while rest > 0:
        candidates = [i for i in range(1, count) if holding[i] < largest] or [i for i in range(1, count) if holding[i] < limit]
        pool, remaining = sum([weights[i] for i in candidates]), rest
        for i in candidates:
            addition = min(limit - holding[i], max(1, remaining * weights[i] // pool), rest)
            holding[i] = holding[i] + addition
            rest = rest - addition
    return np.array(holding)


def centred(stream_key, dims, spread, limit, cuts=(), kind=jnp.bfloat16):
    entries = spread * jax.random.normal(stream_key, dims, jnp.float32)
    if cuts:
        entries = entries * levels(stream_key, dims, cuts, -0.22, 0.18)
    return jnp.clip(entries, -limit, limit).astype(kind)


def setup_inputs(seed: int = 0) -> dict:
    streams_of = jax.random.split(jax.random.key(seed), 13)
    stream = centred(streams_of[0], (TOKENS, D), 1.0, 6.0, ((0, 32),))
    projected = centred(streams_of[1], (TOKENS, D), 1.0, 6.0, ((0, 8), (1, 4)))
    segments = jnp.searchsorted(jnp.cumsum(ragged_sizes(streams_of[2], DOCS, TOKENS, DOC_MOST, 2)), jnp.arange(TOKENS), side="right").astype(jnp.int32)
    group_weight = centred(streams_of[3], (GROUPS, GROUP_WIDTH, GROUP_WIDTH), GROUP_WIDTH ** -0.5, 0.25)
    group_scale = jnp.clip(1.0 + 0.18 * jax.random.normal(streams_of[4], (D,), jnp.float32), 0.1, 1.9)
    out_weight = centred(streams_of[5], (D, D), D ** -0.5, 0.125)
    ffn_gain = jnp.clip(1.0 + 0.18 * jax.random.normal(streams_of[6], (D,), jnp.float32), 0.1, 1.9)
    routes_keys = jax.random.split(jax.random.fold_in(streams_of[7], 1), TOKENS // TOK_DEV)
    routes_turns = jax.random.permutation(jax.random.fold_in(streams_of[7], 3), TOKENS // TOK_DEV)
    routes = jax.vmap(lambda own, number: deal_out(jax.random.fold_in(streams_of[7], 2), own, number, TOK_DEV, EXPERTS, TOP, CAP, 2))(routes_keys, routes_turns).reshape((TOKENS, TOP))
    route_weights = jnp.clip(0.05 + 0.45 * jax.random.uniform(streams_of[8], (TOKENS, TOP), jnp.float32) ** levels(streams_of[8], (TOKENS, TOP), ((0, 32),), -0.2, 0.2), 0.05, 0.5)
    expert_gate = centred(streams_of[9], (EXPERTS, D, FF), (D // 4) ** -0.5, 0.25, ((0, 32),))
    expert_up = centred(streams_of[10], (EXPERTS, D, FF), (D // 4) ** -0.5, 0.25, ((0, 32),))
    expert_down = centred(streams_of[11], (EXPERTS, FF, D), FF ** -0.5, 0.1875, ((0, 32),))
    return {"stream": stream, "projected": projected, "segments": segments, "group_weight": group_weight, "group_scale": group_scale, "out_weight": out_weight, "ffn_gain": ffn_gain, "routes": routes, "route_weights": route_weights, "expert_gate": expert_gate, "expert_up": expert_up, "expert_down": expert_down}


norm_eps = 1e-05
clamp_limit = 7.0
sigmoid_alpha = 1.702
longest_window = 16

def pool_residue(projected, segments):
    length, channels = projected.shape
    values = projected.astype(jnp.float32)
    channel = jnp.arange(channels, dtype=jnp.int32)
    window = jnp.left_shift(jnp.full((channels,), 2, jnp.int32), channel // (channels // GROUPS))
    window_sum = jnp.zeros((length, channels), jnp.float32)
    window_count = jnp.zeros((length, channels), jnp.float32)
    for offset in range(longest_window):
        earlier_rows = jnp.pad(values, ((offset, 0), (0, 0)))[:length]
        earlier_docs = jnp.pad(segments, (offset, 0), constant_values=-1)[:length]
        included = (earlier_docs == segments)[:, None] & (offset < window)[None, :]
        window_sum = window_sum + jnp.where(included, earlier_rows, jnp.float32(0.0))
        window_count = window_count + included.astype(jnp.float32)
    return (window_sum / window_count - values).astype(jnp.bfloat16)

def rms_scale(resid, gain):
    values = resid.astype(jnp.float32)
    inverse = lax.rsqrt(lax.optimization_barrier(jnp.mean(values * values, -1, keepdims=True)) + norm_eps)
    return (values * inverse * gain.astype(jnp.float32)).astype(jnp.bfloat16)

def run_expert(block, gate_matrix, up_matrix, down_matrix):
    leading = block.shape[:-1]
    flat_rows = block.reshape(-1, block.shape[-1])
    gate_value = jnp.dot(flat_rows, gate_matrix, preferred_element_type=jnp.float32)
    up_value = jnp.dot(flat_rows, up_matrix, preferred_element_type=jnp.float32)
    gated = jnp.minimum(gate_value, clamp_limit)
    linear = jnp.clip(up_value, -clamp_limit, clamp_limit)
    activated = (gated * jax.nn.sigmoid(sigmoid_alpha * gated) * (linear + 1.0)).astype(jnp.bfloat16)
    result = jnp.dot(activated, down_matrix, preferred_element_type=jnp.float32).astype(jnp.bfloat16)
    return result.reshape(leading + (down_matrix.shape[1],))

def reference(stream, projected, segments, group_weight, group_scale, out_weight, ffn_gain, routes, route_weights, expert_gate, expert_up, expert_down):
    mixed = pool_residue(projected, segments)
    length, model_width = mixed.shape
    group_width = model_width // GROUPS
    grouped = jnp.einsum('rgc,gcd->rgd', mixed.reshape(length, GROUPS, group_width).astype(jnp.float32), group_weight.astype(jnp.float32)).reshape(length, model_width)
    scaled = (grouped * group_scale.astype(jnp.float32)).astype(jnp.bfloat16)
    mixer_out = jnp.dot(scaled, out_weight, preferred_element_type=jnp.float32)
    resid = (stream.astype(jnp.float32) + mixer_out).astype(jnp.bfloat16)
    normed = rms_scale(resid, ffn_gain)
    flat_routes = routes.reshape(-1)
    flat_weights = route_weights.reshape(-1)
    token_of = jnp.arange(flat_routes.shape[0], dtype=jnp.int32) // TOP
    most_rows = EXPERTS * CAP

    def one_expert(carry, inputs):
        expert_id, gate_matrix, up_matrix, down_matrix = inputs
        matches = flat_routes == expert_id
        picked = jnp.nonzero(matches, size=most_rows, fill_value=0)[0].astype(jnp.int32)
        live = jnp.arange(most_rows, dtype=jnp.int32) < jnp.sum(matches.astype(jnp.int32))
        tokens_in = token_of[picked]
        expert_out = run_expert(normed[tokens_in], gate_matrix, up_matrix, down_matrix)
        weighting = jnp.where(live, flat_weights[picked], jnp.float32(0.0))
        carry = carry.at[tokens_in].add(expert_out.astype(jnp.float32) * weighting[:, None])
        return (carry, None)
    moe_sum, unused = lax.scan(one_expert, jnp.zeros((length, model_width), jnp.float32), (jnp.arange(EXPERTS, dtype=jnp.int32), expert_gate, expert_up, expert_down))
    return (resid.astype(jnp.float32) + moe_sum).astype(jnp.bfloat16)
```

```python
import jax
import jax.numpy as jnp
from jax import lax
from jax.experimental import pallas as pl
from jax.experimental.pallas import tpu as pltpu
from jax.sharding import PartitionSpec as P

GROUPS = 4
CHUNKS = 8
REACH = 2
AHEAD = 2

norm_eps = 1e-05
clamp_limit = 7.0
sigmoid_alpha = 1.702
longest_window = 16


def layer_kernel(
    x_count,
    z_count,
    tp_count,
    capacity,
    share,
    routes_hbm,
    weights_hbm,
    docs_hbm,
    scale_hbm,
    gain_hbm,
    stream_hbm,
    proj_hbm,
    group_hbm,
    outw_hbm,
    gate_hbm,
    up_hbm,
    down_hbm,
    out_hbm,
    routes,
    weights,
    docs,
    prev_docs,
    scale,
    gain,
    stream,
    proj,
    group_ref,
    outw_ref,
    gate_ref,
    up_ref,
    down_ref,
    docs_col,
    mixed,
    gathered,
    scaled,
    squares,
    info,
    column,
    select,
    weigh,
    outgoing,
    rows,
    acc,
    activated,
    returned,
    sums_out,
    sums_in,
    sums_fwd,
    out_ref,
    load_sem,
    out_sem,
    halo_send,
    halo_recv,
    mix_send,
    mix_recv,
    info_send,
    info_recv,
    col_send,
    col_recv,
    plane_send,
    plane_recv,
    back_send,
    back_recv,
    sum_send,
    sum_recv,
    fwd_recv,
):
    sp, tp = lax.axis_index("sp"), lax.axis_index("tp")
    sp_count = x_count * z_count
    z, x = lax.div(sp, x_count), lax.rem(sp, x_count)
    plane = x_count * tp_count
    place = x * tp_count + tp
    tok, width = stream.shape
    channels = proj.shape[1]
    row_count = tok * tp_count
    group_width = group_ref.shape[1]
    top_count = routes.shape[0]
    hidden = gate_ref.shape[1]
    wide = width // CHUNKS
    tiles = hidden // wide
    halo = longest_window
    last = z_count - 1
    slot_count = plane * share
    first_row, last_row = sp > 0, sp < sp_count - 1

    def at_z(step):
        return {"sp": sp + step * x_count, "tp": tp}

    def at_plane(other):
        return {"sp": z * x_count + lax.div(other, tp_count), "tp": lax.rem(other, tp_count)}

    def remote(src, dst, send, recv, device):
        return pltpu.make_async_remote_copy(
            src_ref=src,
            dst_ref=dst,
            send_sem=send,
            recv_sem=recv,
            device_id=device,
            device_id_type=pl.DeviceIdType.MESH,
        )

    def cols_of(k):
        return pl.ds(pl.multiple_of(k * wide, wide), wide)

    def share_of(i):
        return pl.ds(pl.multiple_of(i * share, share), share)

    def block_of(i):
        return pl.ds(pl.multiple_of(i * tok, tok), tok)

    def inside(d, sgn):
        return (z + d <= last) if sgn > 0 else (z >= d)

    def behind(d, sgn):
        return inside(d, -sgn)

    pairs = (
        (proj_hbm, proj.at[pl.ds(halo, row_count)]),
        (docs_hbm, docs),
        (routes_hbm, routes),
        (weights_hbm, weights),
        (group_hbm, group_ref),
        (scale_hbm, scale),
        (gain_hbm, gain),
        (stream_hbm, stream),
        (outw_hbm, outw_ref),
        (gate_hbm, gate_ref),
        (up_hbm, up_ref),
        (down_hbm, down_ref),
    )
    loads = [
        pltpu.make_async_copy(src, dst, load_sem.at[i]) for i, (src, dst) in enumerate(pairs)
    ]
    for load in loads[:8]:
        load.start()

    barrier = pltpu.get_barrier_semaphore()

    def greet(device):
        pl.semaphore_signal(barrier, inc=1, device_id=device, device_id_type=pl.DeviceIdType.MESH)

    pl.when(first_row)(lambda: greet({"sp": sp - 1, "tp": tp}))
    pl.when(last_row)(lambda: greet({"sp": sp + 1, "tp": tp}))

    @pl.loop(1, z_count)
    def _(i):
        greet({"sp": lax.rem(sp + i * x_count, sp_count), "tp": tp})

    @pl.loop(1, plane)
    def _(i):
        greet(at_plane(lax.rem(place + i, plane)))

    for load in loads[8:]:
        load.start()

    loads[2].wait()
    loads[3].wait()
    expert_count = plane * z_count
    expert_ids = lax.broadcasted_iota(jnp.int32, (expert_count, tok), 0)
    named = [
        (expert_ids == routes[j : j + 1, :]).astype(jnp.float32) for j in range(top_count)
    ]
    marks = sum(named[1:], named[0])
    earlier = lax.broadcasted_iota(jnp.int32, (tok, tok), 0) < lax.broadcasted_iota(
        jnp.int32, (tok, tok), 1
    )
    before = jnp.dot(
        marks.astype(jnp.bfloat16),
        jnp.where(earlier, 1.0, 0.0).astype(jnp.bfloat16),
        preferred_element_type=jnp.float32,
    )
    for j in range(top_count):
        rank = jnp.sum(named[j] * before, 0, keepdims=True)
        info[z, j : j + 1, :] = routes[j : j + 1, :].astype(jnp.float32) * share + rank
    info[z, top_count : 2 * top_count, :] = weights[...]

    loads[0].wait()
    loads[1].wait()
    pl.semaphore_wait(
        barrier,
        plane - 1 + last + first_row.astype(jnp.int32) + last_row.astype(jnp.int32),
    )

    def halo_rows(device):
        return remote(
            proj.at[pl.ds(row_count, halo)],
            proj.at[pl.ds(0, halo)],
            halo_send.at[0],
            halo_recv.at[0],
            device,
        )

    def halo_docs(device):
        return remote(docs, prev_docs, halo_send.at[1], halo_recv.at[1], device)

    onward = {"sp": sp + 1, "tp": tp}

    @pl.when(last_row)
    def _():
        halo_rows(onward).start()
        halo_docs(onward).start()

    def info_to(i):
        return remote(
            info.at[z],
            info.at[z],
            info_send.at[i - 1],
            info_recv.at[z],
            {"sp": lax.rem(sp + i * x_count, sp_count), "tp": tp},
        )

    def info_from(i):
        other = lax.rem(z + i, z_count)
        return remote(
            info.at[other],
            info.at[other],
            info_send.at[i - 1],
            info_recv.at[other],
            {"sp": lax.rem(sp + i * x_count, sp_count), "tp": tp},
        )

    @pl.loop(1, z_count)
    def _(i):
        info_to(i).start()

    def spread(row):
        return jnp.broadcast_to(row, (128, row.shape[1])).T

    values = docs[...].astype(jnp.float32)
    for r in range(tp_count):
        docs_col[pl.ds(halo + r * tok, tok), :] = spread(values[r : r + 1, :])
    channel = tp * channels + lax.broadcasted_iota(jnp.int32, (tok + halo, 128), 1)

    def pool_block(r):
        window = pl.ds(r * tok, tok + halo)
        here = docs_col[window, :]
        joins = [
            (here == pltpu.roll(here, 1 << k, 0)) & (channel >= k * group_width)
            for k in range(GROUPS)
        ]
        count = jnp.ones_like(here)
        for k in range(GROUPS):
            count = jnp.where(joins[k], count + pltpu.roll(count, 1 << k, 0), count)
        inverse = 1.0 / count
        for lane in range(0, channels, 128):
            cols = slice(lane, lane + 128)
            own = proj[window, cols].astype(jnp.float32)
            total = own
            for k in range(GROUPS):
                total = jnp.where(joins[k], total + pltpu.roll(total, 1 << k, 0), total)
            mixed[r, :, cols] = (total * inverse - own)[halo:].astype(jnp.bfloat16)

    def mix_to(r):
        return remote(
            mixed.at[r],
            gathered.at[tp],
            mix_send.at[r],
            mix_recv.at[tp],
            {"sp": sp, "tp": r},
        )

    def mix_from(r):
        return remote(
            mixed.at[r],
            gathered.at[r],
            mix_send.at[r],
            mix_recv.at[r],
            {"sp": sp, "tp": r},
        )

    for r in [*range(1, tp_count), 0]:
        if r == 0:

            @pl.when(first_row)
            def _():
                halo_rows(onward).wait_recv()
                halo_docs(onward).wait_recv()
                tail = prev_docs[tp_count - 1 : tp_count, :].astype(jnp.float32)
                docs_col[pl.ds(0, halo), :] = spread(tail)[tok - halo :]

            @pl.when(jnp.logical_not(first_row))
            def _():
                proj[pl.ds(0, halo), :] = jnp.zeros((halo, channels), proj.dtype)
                docs_col[pl.ds(0, halo), :] = jnp.full((halo, 128), -1.0, jnp.float32)

        pool_block(r)
        pl.when(tp != r)(lambda r=r: mix_to(r).start())

        @pl.when(tp == r)
        def _(r=r):
            gathered[r] = mixed[r]

    @pl.loop(1, z_count)
    def _(i):
        info_from(i).wait_recv()

    slot_rows = lax.broadcasted_iota(jnp.int32, (slot_count, tok), 0).astype(jnp.float32)
    slot_cols = lax.broadcasted_iota(jnp.int32, (tok, slot_count), 1).astype(jnp.float32)
    base = (z * slot_count).astype(jnp.float32)

    for s in range(z_count):
        theirs = info[s]
        local = theirs[:top_count] - base
        here = (local >= 0.0) & (local < float(slot_count))
        target = jnp.where(here, local + float(s * capacity), -1.0)
        both = jnp.concatenate([target, theirs[top_count:]], 0)
        turned = both.T
        picks = slot_rows == target[0:1, :]
        for j in range(1, top_count):
            picks = picks | (slot_rows == target[j : j + 1, :])
        select[:, s * tok : (s + 1) * tok] = jnp.where(picks, 1.0, 0.0).astype(jnp.bfloat16)
        share_out = jnp.where(
            slot_cols == turned[:, 0:1], turned[:, top_count : top_count + 1], 0.0
        )
        for j in range(1, top_count):
            share_out = jnp.where(
                slot_cols == turned[:, j : j + 1],
                turned[:, top_count + j : top_count + j + 1],
                share_out,
            )
        weigh[s * tok : (s + 1) * tok, :] = share_out.astype(jnp.bfloat16)

    for i in (4, 5, 6, 7, 8):
        loads[i].wait()
    for r in range(tp_count):
        pl.when(tp != r)(lambda r=r: mix_from(r).wait_recv())
    pieces = group_width // channels
    for g in range(GROUPS):
        grouped = jnp.zeros((tok, group_width), jnp.float32)
        for p in range(pieces):
            grouped += jnp.dot(
                gathered[g * pieces + p],
                group_ref[g, p * channels : (p + 1) * channels, :],
                preferred_element_type=jnp.float32,
            )
        cols = slice(g * group_width, (g + 1) * group_width)
        scaled[:, cols] = (grouped * scale[:, cols]).astype(jnp.bfloat16)
    squares[...] = jnp.zeros_like(squares)

    @pl.loop(0, CHUNKS)
    def _(k):
        cols = cols_of(k)
        mixer_out = jnp.dot(scaled[...], outw_ref[:, cols], preferred_element_type=jnp.float32)
        resid = (stream[:, cols].astype(jnp.float32) + mixer_out).astype(jnp.bfloat16)
        stream[:, cols] = resid
        resid = resid.astype(jnp.float32)
        for lane in range(0, wide, 128):
            part = resid[:, lane : lane + 128]
            squares[...] += part * part

    mean = jnp.sum(squares[...], -1, keepdims=True) * (1.0 / width)
    inverse = lax.rsqrt(mean + norm_eps)

    def own_to(k, d, sgn):
        return remote(
            column.at[k, block_of(z)],
            column.at[k, block_of(z)],
            col_send.at[k, 0 if sgn > 0 else 1, d - 1],
            col_recv.at[k, z],
            at_z(sgn * d),
        )

    def relay(k, d, sgn):
        origin = z - sgn * (d - 1)
        return remote(
            column.at[k, block_of(origin)],
            column.at[k, block_of(origin)],
            col_send.at[k, 0 if sgn > 0 else 1, d - 1],
            col_recv.at[k, origin],
            at_z(sgn),
        )

    def arrival(k, d, sgn):
        origin = z - sgn * d
        return remote(
            column.at[k, block_of(origin)],
            column.at[k, block_of(origin)],
            col_send.at[k, 0 if sgn > 0 else 1, d - 1],
            col_recv.at[k, origin],
            at_z(sgn),
        )

    def send_own(k):
        for d in range(min(REACH, last), 0, -1):
            for sgn in (1, -1):
                pl.when(inside(d, sgn))(lambda d=d, sgn=sgn: own_to(k, d, sgn).start())

    @pl.loop(0, CHUNKS)
    def _(k):
        cols = cols_of(k)
        values = stream[:, cols].astype(jnp.float32)
        column[k, block_of(z), :] = (values * inverse * gain[:, cols]).astype(jnp.bfloat16)
        pl.when(k < AHEAD)(lambda: send_own(k))

    def collect(k):
        for d in range(min(REACH, last), 0, -1):
            for sgn in (1, -1):

                @pl.when(behind(d, sgn))
                def _(d=d, sgn=sgn):
                    arrival(k, d, sgn).wait_recv()
                    if d == REACH and d < last:
                        pl.when(inside(1, sgn))(lambda: relay(k, d + 1, sgn).start())

        for d in range(REACH + 1, z_count):
            for sgn in (1, -1):

                @pl.when(behind(d, sgn))
                def _(d=d, sgn=sgn):
                    arrival(k, d, sgn).wait_recv()
                    if d < last:
                        pl.when(inside(1, sgn))(lambda: relay(k, d + 1, sgn).start())

    def to_expert(k, i):
        other = lax.rem(place + i, plane)
        return remote(
            outgoing.at[k, share_of(other)],
            rows.at[k, share_of(i)],
            plane_send.at[k, i - 1],
            plane_recv.at[k, i - 1],
            at_plane(other),
        )

    def dispatch(k):
        outgoing[k] = jnp.dot(
            select[...], column[k], preferred_element_type=jnp.float32
        ).astype(jnp.bfloat16)

        @pl.loop(1, plane)
        def _(i):
            to_expert(k, i).start()

        rows[k, pl.ds(0, share)] = outgoing[k, share_of(place)]

    def received(k):
        @pl.loop(1, plane)
        def _(i):
            to_expert(k, i).wait_recv()

    def tile_of(n):
        return pl.ds(pl.multiple_of(n * wide, wide), wide)

    def product(k, ref, n):
        return jnp.dot(rows[k], ref[cols_of(k), tile_of(n)], preferred_element_type=jnp.float32)

    def accumulate(k):
        received(k)

        @pl.when(k == 0)
        def _():
            loads[9].wait()
            loads[10].wait()

            @pl.loop(0, tiles)
            def _(n):
                acc[n, 0:slot_count] = product(0, gate_ref, n)
                acc[tiles + n, 0:slot_count] = product(0, up_ref, n)

        @pl.when(k > 0)
        def _():
            @pl.loop(0, tiles)
            def _(n):
                acc[n, 0:slot_count] += product(k, gate_ref, n)
                acc[tiles + n, 0:slot_count] += product(k, up_ref, n)

    @pl.loop(0, CHUNKS)
    def _(k):
        pl.when(k + AHEAD < CHUNKS)(lambda: send_own(k + AHEAD))
        collect(k)
        dispatch(k)
        pl.when(k > 0)(lambda: accumulate(k - 1))

    received(CHUNKS - 1)

    @pl.loop(0, tiles)
    def _(n):
        gate_value = acc[n, 0:slot_count] + product(CHUNKS - 1, gate_ref, n)
        up_value = acc[tiles + n, 0:slot_count] + product(CHUNKS - 1, up_ref, n)
        gated = jnp.minimum(gate_value, clamp_limit)
        linear = jnp.clip(up_value, -clamp_limit, clamp_limit)
        activated[:, tile_of(n)] = (
            gated * jax.nn.sigmoid(sigmoid_alpha * gated) * (linear + 1.0)
        ).astype(jnp.bfloat16)

    loads[11].wait()

    def to_relay(k, i):
        return remote(
            outgoing.at[k, share_of(i)],
            returned.at[k, share_of(place)],
            back_send.at[k, i - 1],
            back_recv.at[k, i - 1],
            at_plane(lax.rem(place + plane - i, plane)),
        )

    @pl.loop(0, CHUNKS)
    def _(k):
        @pl.loop(1, plane)
        def _(i):
            to_expert(k, i).wait_send()

        outgoing[k] = jnp.dot(
            activated[...], down_ref[:, cols_of(k)], preferred_element_type=jnp.float32
        ).astype(jnp.bfloat16)

        @pl.loop(1, plane)
        def _(i):
            to_relay(k, i).start()

        returned[k, share_of(place)] = outgoing[k, pl.ds(0, share)]

    def sum_to(k, d, sgn):
        target = z + sgn * d
        if d <= REACH:
            return remote(
                sums_out.at[k, target],
                sums_in.at[k, z],
                sum_send.at[k, target],
                sum_recv.at[k, z],
                at_z(sgn * d),
            )
        return remote(
            sums_out.at[k, target],
            sums_fwd.at[k, target],
            sum_send.at[k, target],
            fwd_recv.at[k, target],
            at_z(sgn),
        )

    def sum_from(k, d, sgn):
        origin = z - sgn * d
        return remote(
            sums_out.at[k, origin],
            sums_in.at[k, origin],
            sum_send.at[k, origin],
            sum_recv.at[k, origin],
            at_z(-sgn * d),
        )

    def forwarded(k, d, sgn):
        target = z + sgn * d
        return remote(
            sums_out.at[k, target],
            sums_fwd.at[k, target],
            sum_send.at[k, target],
            fwd_recv.at[k, target],
            at_z(-sgn),
        )

    def combine(k):
        @pl.loop(1, plane)
        def _(i):
            to_relay(k, i).wait_recv()

        acc[k, 0 : z_count * tok] = jnp.dot(
            weigh[...], returned[k], preferred_element_type=jnp.float32
        )
        for d in range(last, 0, -1):
            for sgn in (1, -1):

                def emit(d=d, sgn=sgn):
                    sums_out[k, z + sgn * d] = acc[k, block_of(z + sgn * d)].astype(jnp.bfloat16)
                    sum_to(k, d, sgn).start()

                if d < REACH:
                    pl.when(inside(d, sgn))(emit)
                else:
                    pl.when(inside(d, sgn) & jnp.logical_not(behind(1, sgn)))(emit)

    def pass_on(k):
        for d in range(last - 1, REACH - 1, -1):
            for sgn in (1, -1):

                @pl.when(inside(d, sgn) & behind(1, sgn))
                def _(d=d, sgn=sgn):
                    target = z + sgn * d
                    forwarded(k, d, sgn).wait_recv()
                    sums_out[k, target] = (
                        acc[k, block_of(target)] + sums_fwd[k, target].astype(jnp.float32)
                    ).astype(jnp.bfloat16)
                    sum_to(k, d, sgn).start()

    def put_out(k):
        return pltpu.make_async_copy(
            out_ref.at[:, cols_of(k)], out_hbm.at[:, cols_of(k)], out_sem.at[k]
        )

    def finish(k):
        own = block_of(z)
        for d in range(1, min(REACH, last) + 1):
            for sgn in (1, -1):

                @pl.when(behind(d, sgn))
                def _(d=d, sgn=sgn):
                    sum_from(k, d, sgn).wait_recv()
                    acc[k, own] += sums_in[k, z - sgn * d].astype(jnp.float32)

        out_ref[:, cols_of(k)] = (
            stream[:, cols_of(k)].astype(jnp.float32) + acc[k, own]
        ).astype(jnp.bfloat16)
        put_out(k).start()

    @pl.loop(0, CHUNKS)
    def _(k):
        combine(k)
        pl.when(k > 0)(lambda: pass_on(k - 1))
        pl.when(k > 1)(lambda: finish(k - 2))

    pass_on(CHUNKS - 1)
    finish(CHUNKS - 2)
    finish(CHUNKS - 1)

    @pl.when(last_row)
    def _():
        halo_rows(onward).wait_send()
        halo_docs(onward).wait_send()

    @pl.loop(1, z_count)
    def _(i):
        info_to(i).wait_send()

    for r in range(tp_count):
        pl.when(tp != r)(lambda r=r: mix_to(r).wait_send())

    @pl.loop(0, CHUNKS)
    def _(k):
        for d in range(1, z_count):
            for sgn in (1, -1):
                if d <= REACH:
                    pl.when(inside(d, sgn))(lambda d=d, sgn=sgn: own_to(k, d, sgn).wait_send())
                else:

                    @pl.when(behind(d - 1, sgn) & inside(1, sgn))
                    def _(d=d, sgn=sgn):
                        relay(k, d, sgn).wait_send()

                pl.when(inside(d, sgn))(lambda d=d, sgn=sgn: sum_to(k, d, sgn).wait_send())

        @pl.loop(1, plane)
        def _(i):
            to_relay(k, i).wait_send()

        put_out(k).wait()


def body(
    stream,
    projected,
    segments,
    group_weight,
    group_scale,
    out_weight,
    ffn_gain,
    routes,
    route_weights,
    expert_gate,
    expert_up,
    expert_down,
):
    tok, width = stream.shape
    row_count, channels = projected.shape
    sp_count, tp_count = lax.axis_size("sp"), lax.axis_size("tp")
    x_count = max(tp_count // 2, 1)
    z_count = sp_count // x_count
    plane = x_count * tp_count
    top_count = routes.shape[1]
    group_width = group_weight.shape[1]
    hidden = expert_gate.shape[2]
    capacity = 3 * tok * top_count // (2 * plane * z_count)
    share = -(-z_count * capacity // 16) * 16
    slots = plane * share
    wide = width // CHUNKS
    last = max(z_count - 1, 1)
    acc_shape = (max(2 * hidden // wide, CHUNKS), max(slots, z_count * tok), wide)
    bf, f32, i32 = jnp.bfloat16, jnp.float32, jnp.int32
    hbm = pl.BlockSpec(memory_space=pltpu.HBM)
    dma = pltpu.SemaphoreType.DMA
    vmem = pltpu.VMEM
    return pl.pallas_call(
        lambda *refs: layer_kernel(x_count, z_count, tp_count, capacity, share, *refs),
        out_shape=jax.ShapeDtypeStruct((tok, width), bf),
        in_specs=[hbm] * 12,
        out_specs=hbm,
        scratch_shapes=[
            vmem((top_count, tok), i32),
            vmem((top_count, tok), f32),
            vmem((tp_count, tok), i32),
            vmem((tp_count, tok), i32),
            vmem((1, width), f32),
            vmem((1, width), f32),
            vmem((tok, width), bf),
            vmem((longest_window + row_count, channels), bf),
            vmem(group_weight.shape, bf),
            vmem(out_weight.shape, bf),
            vmem((width, hidden), bf),
            vmem((width, hidden), bf),
            vmem((hidden, width), bf),
            vmem((longest_window + row_count, 128), f32),
            vmem((tp_count, tok, channels), bf),
            vmem((tp_count, tok, channels), bf),
            vmem((tok, width), bf),
            vmem((tok, 128), f32),
            vmem((z_count, 2 * top_count, tok), f32),
            vmem((CHUNKS, z_count * tok, wide), bf),
            vmem((slots, z_count * tok), bf),
            vmem((z_count * tok, slots), bf),
            vmem((CHUNKS, slots, wide), bf),
            vmem((CHUNKS, slots, wide), bf),
            vmem(acc_shape, f32),
            vmem((slots, hidden), bf),
            vmem((CHUNKS, slots, wide), bf),
            vmem((CHUNKS, z_count, tok, wide), bf),
            vmem((CHUNKS, z_count, tok, wide), bf),
            vmem((CHUNKS, z_count, tok, wide), bf),
            vmem((tok, width), bf),
            dma((12,)),
            dma((CHUNKS,)),
            dma((2,)),
            dma((2,)),
            dma((tp_count,)),
            dma((tp_count,)),
            dma((last,)),
            dma((z_count,)),
            dma((CHUNKS, 2, last)),
            dma((CHUNKS, z_count)),
            dma((CHUNKS, plane - 1)),
            dma((CHUNKS, plane - 1)),
            dma((CHUNKS, plane - 1)),
            dma((CHUNKS, plane - 1)),
            dma((CHUNKS, z_count)),
            dma((CHUNKS, z_count)),
            dma((CHUNKS, z_count)),
        ],
        compiler_params=pltpu.CompilerParams(
            collective_id=0, has_side_effects=True, vmem_limit_bytes=65000 * 1024
        ),
        name="layer",
    )(
        routes.T,
        route_weights.T,
        segments.reshape(tp_count, tok),
        group_scale.reshape(1, width),
        ffn_gain.reshape(1, width),
        stream,
        projected,
        group_weight,
        out_weight,
        expert_gate[0],
        expert_up[0],
        expert_down[0],
    )


def solution(mesh):
    in_specs = (
        P(("sp", "tp"), None),
        P("sp", "tp"),
        P("sp"),
        P(),
        P(),
        P(),
        P(),
        P(("sp", "tp"), None),
        P(("sp", "tp"), None),
        P(("sp", "tp"), None, None),
        P(("sp", "tp"), None, None),
        P(("sp", "tp"), None, None),
    )
    out_specs = P(("sp", "tp"), None)
    return jax.shard_map(body, mesh=mesh, in_specs=in_specs, out_specs=out_specs, check_vma=False)
```
